256 devices in a mesh: sp: 64 (over z, y, core), tp: 4 (over x).
Axes of the slice: x: 4, y: 4, z: 8, core: 2. Of those that a mesh axis runs over, the one named last changes fastest.
Arguments:
- hidden_state: bfloat16 [8192, 2048], P('sp'), may hold values from -125 to 125
- norm_gain: float32 [2048], replicated, may hold values from 0.1 to 1.9
- route_ids: int32 [8192, 2], P('sp'), may hold values from 0 to 63, all different within a row; in each aligned block of 128 rows (0 to 127, 128 to 255, ...) at most 8 rows name the same one
- route_logits: float32 [8192, 2], P('sp'), may hold values from -6 to 6
- cotangent: bfloat16 [8192, 2048], P('sp'), may hold values from -16 to 16
- w_gate: bfloat16 [64, 2048, 1536], P('sp', None, 'tp'), may hold values from -0.125 to 0.125
- w_up: bfloat16 [64, 2048, 1536], P('sp', None, 'tp'), may hold values from -0.125 to 0.125
- w_down: bfloat16 [64, 1536, 2048], P('sp', 'tp'), may hold values from -0.15625 to 0.15625
- w_out: bfloat16 [2048, 1024], P(None, 'tp'), may hold values from -0.1875 to 0.1875
- query_rows: bfloat16 [8192, 512], P('sp', 'tp'), may hold values from -6 to 6
- key_rows: bfloat16 [8192, 512], P('sp', 'tp'), may hold values from -6 to 6
- value_rows: bfloat16 [8192, 1024], P('sp', 'tp'), may hold values from -6 to 6
- log_decay: float32 [8192, 512], P('sp', 'tp'), may hold values from -1.6 to 0
- head_gain: float32 [1024], P('tp'), may hold values from 0.1 to 1.9
Outputs:
- d_w_gate: bfloat16 [64, 2048, 1536], P('sp', None, 'tp')
- d_w_up: bfloat16 [64, 2048, 1536], P('sp', None, 'tp')
- d_w_down: bfloat16 [64, 1536, 2048], P('sp', 'tp')
- d_w_out: float32 [2048, 1024], P('sp', 'tp')
- d_queries: bfloat16 [8192, 512], P('sp', 'tp')
- d_keys: bfloat16 [8192, 512], P('sp', 'tp')
- d_values: bfloat16 [8192, 1024], P('sp', 'tp')
- d_log_decay: float32 [8192, 512], P('sp', 'tp')
The draws below stay inside these ranges and needn't reach their ends.
Inputs may be any that keep to these rules, and one draw needn't show every extreme that they name: `route_ids`: in the rows of one device each expert is named at most 8 times, a bound that some block reaches; the two experts of a position differ.
All inputs are finite; a program needn't handle non-finite values.
Results may differ from the reference program's by a relative error of at most 0.014.
Values may be sent and summed in bfloat16 or wider, within the bound.
No kernel may reach another device: no remote copies, remote signals or barrier semaphores. Data moves between devices by JAX's collectives and lax.ppermute only.
A program may use at most 128 MiB of HBM per device.

```python
import math
import jax
import jax.numpy as jnp
import numpy as np
from jax import lax

D = 2048
HEADS = 8
KEY_DIM = 64
VAL_DIM = 128
FFE = 1536
BLOCK = 64
TOK_DEV = 128
HK = 512
HV = 1024
EXPERTS = 64
CAP = 8
SEQUENCE_TOKENS = 8192
N_SP = 64
N_TP = 4


def draw_hidden_state(key, part):
    every_key = jax.random.split(key, 3)
    row_scale = jnp.exp(jax.random.uniform(every_key[0], (SEQUENCE_TOKENS, 1), minval=0.0, maxval=math.log(10.0)))
    col_scale = jnp.exp(jax.random.uniform(every_key[1], (1, D), minval=0.0, maxval=math.log(3.0)))
    base_vals = jnp.clip(jax.random.normal(every_key[2], (SEQUENCE_TOKENS, D)), -4.0, 4.0)
    return (base_vals * row_scale * col_scale).astype(jnp.bfloat16)


def draw_log_decay(key, part):
    every_key = jax.random.split(key, 7)
    entire_width = HEADS * KEY_DIM
    order_heads = jax.random.permutation(every_key[0], HEADS)
    slow_count = HEADS // 2
    slow_head = (order_heads < slow_count).astype(jnp.float32)
    slow_chan = jnp.repeat(slow_head, KEY_DIM)[None, :]
    slow_rate = math.log(10.0) / (3.0 * SEQUENCE_TOKENS) * jnp.exp(jax.random.uniform(every_key[1], (1, entire_width), minval=math.log(0.5), maxval=0.0))
    fast_rate = jnp.exp(jax.random.uniform(every_key[2], (1, entire_width), minval=math.log(0.01), maxval=math.log(1.0 / 30.0)))
    baseline_decay_rate = slow_chan * slow_rate + (1.0 - slow_chan) * fast_rate
    block_multiplier = jnp.exp(jax.random.uniform(every_key[3], (SEQUENCE_TOKENS // TOK_DEV, 1), minval=-math.log(2.0), maxval=math.log(2.0)))
    block_multiplier = jnp.repeat(block_multiplier, TOK_DEV, axis=0)
    element_multiplier = jax.random.uniform(every_key[4], (SEQUENCE_TOKENS, entire_width), minval=0.5, maxval=1.5)
    spike_positions = jax.random.randint(every_key[5], (3,), 0, SEQUENCE_TOKENS)
    spike_length = jax.random.uniform(every_key[6], (3, entire_width), minval=math.log(0.5), maxval=math.log(0.8))
    spike_token_hits = (jnp.arange(SEQUENCE_TOKENS)[:, None] == spike_positions[None, :]).astype(jnp.float32)
    spike_count = jnp.dot(spike_token_hits, spike_length)
    return -(baseline_decay_rate * block_multiplier * element_multiplier) + spike_count


def spiked(result, key, source, target, parts, factor):
    owner, partner = [(jnp.arange(result.shape[axis_at]) // (result.shape[axis_at] // parts)).reshape([-1 if axis == axis_at else 1 for axis in range(result.ndim)]) for axis_at in (source, target)]
    chosen = jax.random.permutation(key, parts)[partner]
    strong = (owner == chosen) | (owner == (partner + parts // 2) % parts)
    return jnp.where(strong, factor * result, result)


def steps_of(stream_key, extent, cuts, low, high):
    level = 1.0
    for position, blocks in cuts:
        steps = jax.random.uniform(jax.random.fold_in(jax.random.fold_in(stream_key, 6), position), (blocks,), jnp.float32, low / len(cuts), high / len(cuts))
        level = level * jnp.repeat(jnp.exp(steps), extent[position] // blocks).reshape((-1,) + (1,) * (len(extent) - 1 - position))
    return level


def deal_out(stream_key, own, number, rows, number_of, top, limit, slope):
    ranking = jax.random.permutation(stream_key, number_of)
    heavy_load, ordinary = shares(number_of, rows * top, limit, slope, True), shares(number_of, rows * top, limit, slope, False)
    places = jnp.arange(number_of)

    def named(lengths, offset_by):
        used = int((lengths > 0).sum())
        fixed = max(1, used // 4)
        shifted = fixed + (places - fixed + offset_by * (used - fixed)) % max(1, number_of - fixed)
        return jnp.zeros((number_of,), jnp.int32).at[ranking[jnp.where(places < fixed, places, shifted)]].set(jnp.asarray(lengths, jnp.int32))

    lengths = jnp.where(number % 4 == 0, named(heavy_load, number // 4), named(ordinary, number - number // 4 - 1))
    mixed = jax.random.permutation(jax.random.fold_in(own, 3), number_of)
    donor, taker = mixed[0:number_of // 2 * 2:2], mixed[1:number_of // 2 * 2:2]
    room = jnp.minimum(lengths[donor] - 1, limit - lengths[taker]) // 2
    room = jnp.where((donor == ranking[0]) | (taker == ranking[0]) | (lengths[taker] == 0), 0, jnp.maximum(room, 0))
    shifted = jax.random.randint(jax.random.fold_in(own, 4), (number_of // 2,), 0, 1 << 20) % (room + 1)
    lengths = lengths.at[donor].add(-shifted).at[taker].add(shifted)
    labels = jnp.searchsorted(jnp.cumsum(lengths), jnp.arange(rows * top), side="right").astype(jnp.int32)
    listing = labels.reshape(top, rows).T
    listing = listing[jax.random.permutation(jax.random.fold_in(own, 1), rows)]
    offset_by = jax.random.randint(jax.random.fold_in(own, 2), (rows, 1), 0, top)
    return jnp.take_along_axis(listing, (jnp.arange(top)[None, :] + offset_by) % top, axis=1)


def shares(number_of, total, most, skew, full):
    weights = [(1 << 20) // math.isqrt(standing ** skew) + 1 for standing in range(1, number_of + 1)]
    largest = most if full else min(most, max(-(-total // number_of), total * weights[0] // sum(weights)))
    least = 1 if total - largest >= number_of - 1 else 0
    given, spare = [largest] + [least] * (number_of - 1), total - largest - least * (number_of - 1)
    while spare > 0:
        candidates = [i for i in range(1, number_of) if given[i] < largest] or [i for i in range(1, number_of) if given[i] < most]
        whole, left = sum([weights[i] for i in candidates]), spare
        for i in candidates:
            extra = min(most - given[i], max(1, left * weights[i] // whole), spare)
            given[i] = given[i] + extra
            spare = spare - extra
    return np.array(given)


def noise(own_key, shape, scale, most, cuts=(), held_as=jnp.bfloat16):
    result = scale * jax.random.normal(own_key, shape, jnp.float32)
    if cuts:
        result = result * steps_of(own_key, shape, cuts, -0.22, 0.18)
    return jnp.clip(result, -most, most).astype(held_as)


def noise_with(own_key, shape, spread, reach, cuts, heavy, kind=jnp.bfloat16):
    drawn = spread * jax.random.normal(own_key, shape, jnp.float32)
    if cuts:
        drawn = drawn * steps_of(own_key, shape, cuts, -0.22, 0.18)
    return jnp.clip(spiked(drawn, jax.random.fold_in(own_key, 3), *heavy), -reach, reach).astype(kind)


def setup_inputs(seed: int = 0) -> dict:
    streams_of = jax.random.split(jax.random.key(seed), 15)
    hidden_state = draw_hidden_state(jax.random.fold_in(streams_of[14], 71), 0)
    norm_gain = jnp.clip(1.0 + 0.18 * jax.random.normal(streams_of[1], (D,), jnp.float32), 0.1, 1.9)
    route_ids_keys = jax.random.split(jax.random.fold_in(streams_of[2], 1), SEQUENCE_TOKENS // TOK_DEV)
    route_ids_turns = jax.random.permutation(jax.random.fold_in(streams_of[2], 3), SEQUENCE_TOKENS // TOK_DEV)
    route_ids = jax.vmap(lambda own, number: deal_out(jax.random.fold_in(streams_of[2], 2), own, number, TOK_DEV, EXPERTS, 2, CAP, 1))(route_ids_keys, route_ids_turns).reshape((SEQUENCE_TOKENS, 2))
    route_logits = noise(streams_of[3], (SEQUENCE_TOKENS, 2), 1.0, 6.0, ((0, 64),), jnp.float32)
    cotangent = noise_with(streams_of[4], (SEQUENCE_TOKENS, D), 1.0, 16.0, ((0, 64),), (0, 1, 64, 4.0))
    w_gate = noise(streams_of[5], (EXPERTS, D, FFE), D ** -0.5, 0.125, ((0, 64), (2, 4)))
    w_up = noise(streams_of[6], (EXPERTS, D, FFE), D ** -0.5, 0.125, ((0, 64), (2, 4)))
    w_down = noise(streams_of[7], (EXPERTS, FFE, D), FFE ** -0.5, 0.15625, ((0, 64), (1, 4)))
    w_out = noise(streams_of[8], (D, HV), HV ** -0.5, 0.1875, ((1, 4),))
    query_rows = noise(streams_of[9], (SEQUENCE_TOKENS, HK), 1.0, 6.0, ((0, 64), (1, 4)))
    key_rows = noise(streams_of[10], (SEQUENCE_TOKENS, HK), 1.0, 6.0, ((0, 64), (1, 4)))
    value_rows = noise(streams_of[11], (SEQUENCE_TOKENS, HV), 1.0, 6.0, ((0, 64), (1, 4)))
    log_decay = draw_log_decay(jax.random.fold_in(streams_of[14], 71), 0)
    head_gain = jnp.clip(1.0 + 0.18 * jax.random.normal(streams_of[13], (HV,), jnp.float32), 0.1, 1.9)
    return {"hidden_state": hidden_state, "norm_gain": norm_gain, "route_ids": route_ids, "route_logits": route_logits, "cotangent": cotangent, "w_gate": w_gate, "w_up": w_up, "w_down": w_down, "w_out": w_out, "query_rows": query_rows, "key_rows": key_rows, "value_rows": value_rows, "log_decay": log_decay, "head_gain": head_gain}


exact_numeric_mode = lax.Precision.HIGHEST
eps_value = 1e-06

def blocks_of(array, width):
    return array.reshape((array.shape[0] // BLOCK, BLOCK, array.shape[1] // width, width))

def gla_forward(query_f, key_f, value_f, log_f):
    causal = jnp.arange(BLOCK)[:, None] >= jnp.arange(BLOCK)[None, :]

    def advance(carried_state, inputs):
        query_block, key_block, value_block, log_b = inputs
        cumulative_decay = jnp.cumsum(log_b, axis=0)
        decay_mid = cumulative_decay[BLOCK // 2]
        final_decay = cumulative_decay[BLOCK - 1]
        scores = jnp.einsum('thk,shk->hts', query_block * jnp.exp(cumulative_decay - decay_mid), key_block * jnp.exp(decay_mid - cumulative_decay), precision=exact_numeric_mode)
        scores = jnp.where(causal[None], scores, 0.0)
        result_output = jnp.einsum('hts,shv->thv', scores, value_block, precision=exact_numeric_mode)
        result_output = result_output + jnp.einsum('jml,mld->jmd', query_block * jnp.exp(cumulative_decay), carried_state, precision=exact_numeric_mode)
        updated_state = jnp.exp(final_decay)[:, :, None] * carried_state + jnp.einsum('yiu,yig->iug', key_block * jnp.exp(final_decay - cumulative_decay), value_block, precision=exact_numeric_mode)
        return (updated_state, result_output)
    zero_state = jnp.zeros((HEADS, KEY_DIM, VAL_DIM), jnp.float32)
    final_state, outputs = lax.scan(advance, zero_state, (blocks_of(query_f, KEY_DIM), blocks_of(key_f, KEY_DIM), blocks_of(value_f, VAL_DIM), blocks_of(log_f, KEY_DIM)))
    return outputs.reshape(SEQUENCE_TOKENS, HEADS, VAL_DIM)

def slot_numbers(ids):
    flat_ids = ids.reshape(-1)
    one_hot = (flat_ids[:, None] == jnp.arange(EXPERTS, dtype=jnp.int32)[None, :]).astype(jnp.int32)
    slot_rank = lax.optimization_barrier(jnp.sum((jnp.cumsum(one_hot, axis=0) - 1) * one_hot, axis=1))
    return (flat_ids * CAP + slot_rank).astype(jnp.int32)

def slot_sources(slots):
    row_total = slots.shape[0]
    return jnp.full((EXPERTS * CAP,), row_total, jnp.int32).at[slots].set(jnp.arange(row_total, dtype=jnp.int32))

def reference(hidden_state, norm_gain, route_ids, route_logits, cotangent, w_gate, w_up, w_down, w_out, query_rows, key_rows, value_rows, log_decay, head_gain):
    gain_heads = head_gain.reshape(HEADS, VAL_DIM)

    def mixer_fwd(query_f, key_f, value_f, log_f):
        head_out = gla_forward(query_f, key_f, value_f, log_f)
        inv_rms = lax.rsqrt(lax.optimization_barrier(jnp.mean(head_out * head_out, axis=-1, keepdims=True)) + eps_value)
        return (head_out * inv_rms * gain_heads).reshape(SEQUENCE_TOKENS, HEADS * VAL_DIM)
    mixed_f, pullback = jax.vjp(mixer_fwd, query_rows.astype(jnp.float32), key_rows.astype(jnp.float32), value_rows.astype(jnp.float32), log_decay)
    mixed_out = mixed_f.astype(jnp.bfloat16)
    state_f = hidden_state.astype(jnp.float32)
    row_scale = lax.rsqrt(lax.optimization_barrier(jnp.mean(state_f * state_f, axis=-1, keepdims=True)) + eps_value)
    unit_rows = state_f * row_scale
    normed_in = (unit_rows * norm_gain).astype(jnp.bfloat16)
    route_weight = jax.nn.softmax(route_logits, axis=-1)
    cot_f = cotangent.astype(jnp.float32)
    slot_grads = (route_weight[:, :, None] * cot_f[:, None, :]).astype(jnp.bfloat16).reshape(2 * SEQUENCE_TOKENS, D)
    slots = jax.vmap(slot_numbers)(route_ids.reshape(N_SP, TOK_DEV, 2))
    sources = jax.vmap(slot_sources)(slots)
    offsets = (jnp.arange(N_SP, dtype=jnp.int32) * (2 * TOK_DEV))[:, None]
    global_src = jnp.where(sources < 2 * TOK_DEV, sources + offsets, 2 * SEQUENCE_TOKENS).astype(jnp.int32)
    by_expert = global_src.reshape(N_SP, EXPERTS, CAP).transpose(1, 0, 2).reshape(EXPERTS, N_SP * CAP)
    padded_in = jnp.concatenate([normed_in, jnp.zeros((1, D), jnp.bfloat16)], axis=0)
    padded_grad = jnp.concatenate([slot_grads, jnp.zeros((1, D), jnp.bfloat16)], axis=0)
    part_width = FFE // N_TP

    def one_expert(returned, inputs):
        rows_src, gate_w, up_w, down_w = inputs
        rows_in = padded_in[jnp.where(rows_src < 2 * SEQUENCE_TOKENS, rows_src // 2, SEQUENCE_TOKENS).astype(jnp.int32)]
        rows_grad = padded_grad[rows_src]
        gate_pre = jnp.dot(rows_in, gate_w, preferred_element_type=jnp.float32)
        up_pre = jnp.dot(rows_in, up_w, preferred_element_type=jnp.float32)
        gate_sig = jax.nn.sigmoid(gate_pre)
        silu_gate = gate_pre * gate_sig
        hidden_units = (silu_gate * up_pre).astype(jnp.bfloat16)
        grad_down = jnp.dot(hidden_units.T, rows_grad, preferred_element_type=jnp.float32)
        grad_hidden = jnp.dot(rows_grad, down_w.T, preferred_element_type=jnp.float32)
        grad_gate_pre = (grad_hidden * up_pre * gate_sig * (1.0 + gate_pre * (1.0 - gate_sig))).astype(jnp.bfloat16)
        grad_up_pre = (grad_hidden * silu_gate).astype(jnp.bfloat16)
        grad_gate = jnp.dot(rows_in.T, grad_gate_pre, preferred_element_type=jnp.float32)
        grad_up = jnp.dot(rows_in.T, grad_up_pre, preferred_element_type=jnp.float32)
        summed_rows = jnp.zeros((N_SP * CAP, D), jnp.float32)
        for group_index in range(N_TP):
            lower = group_index * part_width
            upper = lower + part_width
            partial_piece = jnp.dot(grad_gate_pre[:, lower:upper], gate_w[:, lower:upper].T, preferred_element_type=jnp.float32)
            partial_piece = partial_piece + jnp.dot(grad_up_pre[:, lower:upper], up_w[:, lower:upper].T, preferred_element_type=jnp.float32)
            rounded_piece = lax.optimization_barrier(partial_piece.astype(jnp.bfloat16))
            summed_rows = summed_rows + rounded_piece.astype(jnp.float32)
        returned = returned.at[rows_src].set(summed_rows.astype(jnp.bfloat16), mode='drop')
        return (returned, (grad_gate.astype(jnp.bfloat16), grad_up.astype(jnp.bfloat16), grad_down.astype(jnp.bfloat16)))
    slot_back, expert_grads = lax.scan(one_expert, jnp.zeros((2 * SEQUENCE_TOKENS, D), jnp.bfloat16), (by_expert, w_gate, w_up, w_down))
    grad_normed = lax.optimization_barrier(jnp.sum(slot_back.astype(jnp.float32).reshape(SEQUENCE_TOKENS, 2, D), axis=1))
    grad_unit = grad_normed * norm_gain
    grad_state = row_scale * (grad_unit - unit_rows * lax.optimization_barrier(jnp.mean(grad_unit * unit_rows, axis=-1, keepdims=True)))
    grad_mixed = (cot_f + grad_state).astype(jnp.bfloat16)
    grad_out_w = jnp.dot(grad_mixed.T, mixed_out, preferred_element_type=jnp.float32)
    grad_mix = jnp.dot(grad_mixed, w_out, preferred_element_type=jnp.float32).astype(jnp.bfloat16)
    grad_mix = lax.optimization_barrier(grad_mix).astype(jnp.float32)
    grad_query, grad_key, grad_value, grad_log = pullback(grad_mix)
    return (expert_grads[0], expert_grads[1], expert_grads[2], grad_out_w, grad_query.astype(jnp.bfloat16), grad_key.astype(jnp.bfloat16), grad_value.astype(jnp.bfloat16), grad_log)
```

```python
import jax
import jax.numpy as jnp
from jax import lax
from jax.experimental import pallas as pl
from jax.experimental.pallas import tpu as pltpu
from jax.sharding import Mesh
from jax.sharding import PartitionSpec as P

KEY_DIM = 64
VAL_DIM = 128
BLOCK = 64
SP = ("sp_0", "sp_1", "sp_2")
GROUP = ("sp_1", "sp_2")
N_TP = 4
N_Z = 8
HIGH = lax.Precision.HIGHEST
EPS = 1e-06
F32 = jnp.float32
BF16 = jnp.bfloat16


def exchange(array, axis):
    return lax.all_to_all(array, axis, split_axis=0, concat_axis=0, tiled=True)


def shifted(array, by):
    return lax.ppermute(array, "tp", [((k + by) % N_TP, k) for k in range(N_TP)])


def whole():
    return pl.BlockSpec(memory_space=pltpu.VMEM)


def scalars():
    return pl.BlockSpec(memory_space=pltpu.SMEM)


def run(kernel, name, outs, numbers, *arrays):
    numbers = jnp.stack(numbers) if numbers else jnp.zeros((1,), jnp.int32)
    return pl.pallas_call(
        kernel,
        out_shape=tuple(jax.ShapeDtypeStruct(shape, dtype) for shape, dtype in outs),
        in_specs=[scalars()] + [whole()] * len(arrays),
        out_specs=tuple(whole() for _ in outs),
        name=name,
    )(numbers, *arrays)


def iota(shape, dim):
    return lax.broadcasted_iota(jnp.int32, shape, dim)


def exact(a, b, dims):
    return lax.dot_general(a, b, (dims, ((), ())), precision=HIGH, preferred_element_type=F32)


NN = ((1,), (0,))
NT = ((1,), (1,))
TN = ((0,), (0,))


def paired(a, b, dims):
    return lax.dot_general(a, b, (dims, ((), ())), preferred_element_type=F32)


def dispatch_kernel(rank_ref, hidden_ref, gain_ref, ids_ref, logits_ref, cot_ref, send_ref, place_ref):
    rank = rank_ref[0]
    tok, width = hidden_ref.shape
    quarter = width // 4
    state = hidden_ref[...].astype(F32)
    scale = lax.rsqrt(jnp.mean(state * state, axis=-1, keepdims=True) + EPS)
    normed = ((state * scale) * gain_ref[...]).astype(BF16)
    logits = logits_ref[...]
    l0, l1 = logits[:, 0:1], logits[:, 1:2]
    top = jnp.maximum(l0, l1)
    e0, e1 = jnp.exp(l0 - top), jnp.exp(l1 - top)
    total = e0 + e1
    cot = cot_ref[...].astype(F32)
    grads = [((e / total) * cot).astype(BF16) for e in (e0, e1)]
    rows_all = send_ref.shape[0]
    experts = rows_all // 8
    ids = ids_ref[...]
    eye = iota((experts, tok), 0)
    hot = [(eye == ids[r : r + 1, :]).astype(F32) for r in range(2)]
    earlier = (iota((tok, tok), 0) < iota((tok, tok), 1)).astype(F32)
    before = paired(hot[0] + hot[1], earlier, NN)
    rows = iota((rows_all, tok), 0)
    kept, places = [], []
    for r in range(2):
        slot = jnp.sum(before * hot[r], axis=0, keepdims=True).astype(jnp.int32)
        block = slot >> 1
        first = 8 * ids[r : r + 1, :] + (slot & 1)
        kept.append(jnp.where(block == rank, first, -8))
        places.append(first + 2 * ((block - rank) & 3))
    place_ref[...] = jnp.concatenate(places, axis=0)
    total_in, total_grad = None, None
    for h in range(4):
        pick = [(rows == kept[r] + 2 * h).astype(F32) for r in range(2)]
        lanes = slice(h * quarter, (h + 1) * quarter)
        term = paired((pick[0] + pick[1]).astype(BF16), normed[:, lanes], NN)
        total_in = term if total_in is None else total_in + term
        term = paired(pick[0].astype(BF16), grads[0][:, lanes], NN)
        term = term + paired(pick[1].astype(BF16), grads[1][:, lanes], NN)
        total_grad = term if total_grad is None else total_grad + term
    send_ref[:, :quarter] = total_in.astype(BF16)
    send_ref[:, quarter:] = total_grad.astype(BF16)


def unpack_kernel(_, got_ref, out_ref):
    got = got_ref[...]
    rows, width = out_ref.shape
    quarter = width // 8
    line = iota((rows, got.shape[0]), 0)
    col = iota((rows, got.shape[0]), 1)
    for h in range(4):
        pick = (col == 8 * (line >> 1) + 2 * h + (line & 1)).astype(F32).astype(BF16)
        both = paired(pick, got, NN).astype(BF16)
        out_ref[:, h * quarter : (h + 1) * quarter] = both[:, :quarter]
        out_ref[:, (4 + h) * quarter : (5 + h) * quarter] = both[:, quarter:]


def combine_kernel(_, own_ref, one_ref, two_ref, three_ref, out_ref):
    rows = own_ref.shape[0] // 4
    line = iota((4 * rows, rows), 0)
    col = iota((4 * rows, rows), 1)
    total = None
    for k in range(4):
        acc = own_ref[k * rows : (k + 1) * rows].astype(F32)
        for by, ref in ((1, one_ref), (2, two_ref), (3, three_ref)):
            m = (k + by) % 4
            acc = acc + ref[m * rows : (m + 1) * rows].astype(F32)
        spread = (line == 8 * (col >> 1) + 2 * k + (col & 1)).astype(F32).astype(BF16)
        term = paired(spread, acc.astype(BF16), NN)
        total = term if total is None else total + term
    out_ref[...] = total.astype(BF16)


def pick_kernel(_, returned_ref, place_ref, out_ref):
    tok = out_ref.shape[0]
    slots = iota((returned_ref.shape[0], tok), 0)
    here = ((slots == place_ref[0:1, :]) | (slots == place_ref[1:2, :])).astype(F32).astype(BF16)
    out_ref[...] = paired(here, returned_ref[...], TN).astype(BF16)


def by_head(x):
    half = x.shape[0] // 2
    return jnp.concatenate([x[:half, :VAL_DIM], x[half:, VAL_DIM:]], axis=0)


def spread_heads(x):
    half = x.shape[0] // 2
    zero = jnp.zeros((half, VAL_DIM), F32)
    return jnp.concatenate(
        [jnp.concatenate([x[:half], zero], axis=1), jnp.concatenate([zero, x[half:]], axis=1)], axis=0
    )


def same_block(t, s):
    return (t // BLOCK) == (s // BLOCK)


def mids(cum):
    tok, keys = cum.shape
    row = iota((tok, keys), 0)
    mid = jnp.where(row < BLOCK, cum[BLOCK // 2 : BLOCK // 2 + 1], cum[BLOCK + BLOCK // 2 : BLOCK + BLOCK // 2 + 1])
    last = jnp.where(row < BLOCK, cum[BLOCK - 1 : BLOCK], cum[2 * BLOCK - 1 : 2 * BLOCK])
    return mid, last


def pack_state(out_ref, state, log_row):
    keys = state.shape[0]
    high = log_row.astype(BF16).astype(F32)
    rest = log_row - high
    middle = rest.astype(BF16).astype(F32)
    low = rest - middle
    line = iota((16, state.shape[1]), 0)
    extra = jnp.where(line == 0, high, jnp.where(line == 1, middle, jnp.where(line == 2, low, 0.0)))
    block = state.astype(BF16)
    extra = extra.astype(BF16)
    for k in range(out_ref.shape[0]):
        out_ref[k, :keys, :] = block
        out_ref[k, keys:, :] = extra


def local_kernel(_, key_ref, value_ref, log_ref, pack_ref, cum_ref, cols_ref, first_ref, end_ref):
    tok, keys = key_ref.shape
    logs = log_ref[...]
    t, s = iota((tok, tok), 0), iota((tok, tok), 1)
    lower = ((t >= s) & same_block(t, s)).astype(F32)
    cum = exact(lower, logs, NN)
    cum_ref[...] = cum
    _, last = mids(cum)
    chosen = ((t // BLOCK) == s).astype(F32)
    cols = exact(logs, chosen, TN)
    cols_ref[...] = cols
    key_end = key_ref[...].astype(F32) * jnp.exp(last - cum)
    value = value_ref[...].astype(F32)
    first = by_head(exact(key_end[:BLOCK], value[:BLOCK], TN))
    second = by_head(exact(key_end[BLOCK:], value[BLOCK:], TN))
    end = jnp.exp(cols[:, 1:2]) * first + second
    first_ref[...] = first
    end_ref[...] = end
    pack_state(pack_ref, end, cum[BLOCK - 1 : BLOCK] + cum[2 * BLOCK - 1 : 2 * BLOCK])


def log_rows(got_ref, keys):
    return jnp.concatenate(
        [
            jnp.sum(got_ref[k, keys:, :].astype(F32), axis=0, keepdims=True)
            for k in range(got_ref.shape[0])
        ],
        axis=0,
    )


def walked(term_of, decays, position, length, reverse):
    carried = jnp.zeros((decays.shape[0], VAL_DIM), F32)
    here = carried
    for k in reversed(range(length)) if reverse else range(length):
        here = jnp.where(position == k, carried, here)
        carried = decays[:, k : k + 1] * carried + term_of(k)
    return here, carried


def group_kernel(spot_ref, got_ref, pack_ref, before_ref, cols_ref):
    length, _, keys = got_ref.shape
    rows = log_rows(got_ref, keys)
    cols = jnp.transpose(rows)
    cols_ref[...] = cols
    here, carried = walked(
        lambda k: got_ref[k, :keys, :].astype(F32), jnp.exp(cols), spot_ref[0], length, False
    )
    before_ref[...] = here
    pack_state(pack_ref, carried, jnp.sum(rows, axis=0, keepdims=True))


def forward_kernel(
    spot_ref,
    got_ref,
    before_ref,
    group_ref,
    query_ref,
    key_ref,
    value_ref,
    cum_ref,
    cols_ref,
    first_ref,
    out_ref,
    state_ref,
    zcols_ref,
):
    length, _, keys = got_ref.shape
    cols = jnp.transpose(log_rows(got_ref, keys))
    zcols_ref[...] = cols
    before_z, _ = walked(
        lambda k: got_ref[k, :keys, :].astype(F32), jnp.exp(cols), spot_ref[1], length, False
    )
    group = group_ref[...]
    lead = jnp.sum(jnp.where(iota(group.shape, 1) < spot_ref[0], group, 0.0), axis=1, keepdims=True)
    state = before_ref[...] + jnp.exp(lead) * before_z
    state_ref[...] = state
    cum = cum_ref[...]
    tok = cum.shape[0]
    mid, _ = mids(cum)
    query = query_ref[...].astype(F32)
    query_in = query * jnp.exp(cum - mid)
    key_in = key_ref[...].astype(F32) * jnp.exp(mid - cum)
    value = value_ref[...].astype(F32)
    start = query * jnp.exp(cum)
    t, s = iota((tok, tok), 0), iota((tok, tok), 1)
    causal = (t >= s) & same_block(t, s)
    lane = iota((tok, keys), 1) // KEY_DIM
    later = first_ref[...] + jnp.exp(cols_ref[:, 0:1]) * state
    outside = jnp.concatenate(
        [exact(start[:BLOCK], spread_heads(state), NN), exact(start[BLOCK:], spread_heads(later), NN)],
        axis=0,
    )
    for h in range(2):
        lanes = slice(h * VAL_DIM, (h + 1) * VAL_DIM)
        scores = exact(jnp.where(lane == h, query_in, 0.0), key_in, NT)
        scores = jnp.where(causal, scores, 0.0)
        out_ref[:, lanes] = exact(scores, value[:, lanes], NN) + outside[:, lanes]


def head_norm(head_out, gain):
    normed, scale = [], []
    for h in range(2):
        x = head_out[:, h * VAL_DIM : (h + 1) * VAL_DIM]
        r = lax.rsqrt(jnp.mean(x * x, axis=-1, keepdims=True) + EPS)
        scale.append(r)
        normed.append(x * r)
    return normed, scale


def mixer_kernel(
    rank_ref,
    own_ref,
    one_ref,
    two_ref,
    three_ref,
    hidden_ref,
    cot_ref,
    gain_ref,
    w_out_ref,
    head_ref,
    head_gain_ref,
    query_ref,
    cum_ref,
    cols_ref,
    pack_ref,
    grad_ref,
    adj_ref,
    mixed_ref,
):
    rank = rank_ref[0]
    tok, width = hidden_ref.shape
    part = width // 4
    state = hidden_ref[...].astype(F32)
    scale = lax.rsqrt(jnp.mean(state * state, axis=-1, keepdims=True) + EPS)
    parts = (own_ref, one_ref, two_ref, three_ref)
    inner = jnp.zeros((tok, 1), F32)
    for k in range(4):
        at = pl.multiple_of(((rank + k) & 3) * part, part)
        unit = hidden_ref[:, pl.ds(at, part)].astype(F32) * scale
        u = parts[k][...].astype(F32) * gain_ref[:, pl.ds(at, part)]
        inner = inner + jnp.sum(u * unit, axis=-1, keepdims=True)
    inner = inner / width
    grad_mix = None
    for k in range(4):
        at = pl.multiple_of(((rank + k) & 3) * part, part)
        unit = hidden_ref[:, pl.ds(at, part)].astype(F32) * scale
        u = parts[k][...].astype(F32) * gain_ref[:, pl.ds(at, part)]
        mixed = (cot_ref[:, pl.ds(at, part)].astype(F32) + scale * (u - unit * inner)).astype(BF16)
        mixed_ref[:, pl.ds(at, part)] = mixed
        term = paired(mixed, w_out_ref[pl.ds(at, part), :], NN)
        grad_mix = term if grad_mix is None else grad_mix + term
    grad_mix = grad_mix.astype(BF16).astype(F32)
    head_gain = head_gain_ref[...]
    normed, head_scale = head_norm(head_ref[...], head_gain)
    out = []
    for h in range(2):
        lanes = slice(h * VAL_DIM, (h + 1) * VAL_DIM)
        u = grad_mix[:, lanes] * head_gain[:, lanes]
        n = normed[h]
        out.append(head_scale[h] * (u - n * jnp.mean(u * n, axis=-1, keepdims=True)))
    grad = jnp.concatenate(out, axis=1)
    grad_ref[...] = grad
    start = query_ref[...].astype(F32) * jnp.exp(cum_ref[...])
    early = by_head(exact(start[:BLOCK], grad[:BLOCK], TN))
    late = by_head(exact(start[BLOCK:], grad[BLOCK:], TN))
    adj_ref[...] = late
    local = (jnp.exp(cols_ref[:, 0:1]) * late + early).astype(BF16)
    half = local.shape[0] // 2
    n_g, rows, _ = pack_ref.shape
    n_z = N_Z
    each = (rows - half) // n_z
    state_rows = jnp.concatenate([local[:half], local[half:]], axis=1)
    mixed_out = jnp.concatenate(
        [normed[h] * head_gain[:, h * VAL_DIM : (h + 1) * VAL_DIM] for h in range(2)], axis=1
    ).astype(BF16)
    out_part = paired(mixed_ref[...], mixed_out, TN).astype(BF16)

    for q in range(n_g):
        for z in range(n_z):
            at = (z * n_g + q) * each
            pack_ref[q, z * each : (z + 1) * each, :] = out_part[at : at + each]
        pack_ref[q, n_z * each :, :] = state_rows


def states_of(rows):
    return jnp.concatenate([rows[:, :VAL_DIM], rows[:, VAL_DIM:]], axis=0).astype(F32)


def behind_kernel(spot_ref, got_ref, cols_ref, pack_ref, after_ref):
    length, rows, _ = got_ref.shape
    n_z, each = pack_ref.shape[0], pack_ref.shape[1]
    half = after_ref.shape[0] // 2
    each = each - half
    total = got_ref[0, : rows - half, :].astype(F32)
    for k in range(1, length):
        total = total + got_ref[k, : rows - half, :].astype(F32)
    total = total.astype(BF16)
    here, carried = walked(
        lambda k: states_of(got_ref[k, rows - half :, :]), jnp.exp(cols_ref[...]), spot_ref[0], length, True
    )
    after_ref[...] = here
    carried = carried.astype(BF16)
    state_rows = jnp.concatenate([carried[:half], carried[half:]], axis=1)
    for z in range(n_z):
        pack_ref[z, :each, :] = total[z * each : (z + 1) * each]
        pack_ref[z, each:, :] = state_rows


def inner_kernel(
    _,
    query_ref,
    key_ref,
    value_ref,
    cum_ref,
    cols_ref,
    first_ref,
    state_ref,
    grad_ref,
    dq_ref,
    dk_ref,
    dv_ref,
    dlog_ref,
):
    cum = cum_ref[...]
    tok, keys = cum.shape
    mid, _ = mids(cum)
    query, key = query_ref[...].astype(F32), key_ref[...].astype(F32)
    rise, fall = jnp.exp(cum - mid), jnp.exp(mid - cum)
    query_in, key_in = query * rise, key * fall
    value, grad = value_ref[...].astype(F32), grad_ref[...]
    t, s = iota((tok, tok), 0), iota((tok, tok), 1)
    causal = (t >= s) & same_block(t, s)
    lane = iota((tok, keys), 1) // KEY_DIM
    state = state_ref[...]
    later = first_ref[...] + jnp.exp(cols_ref[:, 0:1]) * state
    outside = jnp.concatenate(
        [exact(grad[:BLOCK], spread_heads(state), NT), exact(grad[BLOCK:], spread_heads(later), NT)],
        axis=0,
    )
    dq = jnp.zeros((tok, keys), F32)
    dk = jnp.zeros((tok, keys), F32)
    for h in range(2):
        lanes = slice(h * VAL_DIM, (h + 1) * VAL_DIM)
        mine = lane == h
        dots = jnp.where(causal, exact(grad[:, lanes], value[:, lanes], NT), 0.0)
        scores = jnp.where(causal, exact(jnp.where(mine, query_in, 0.0), key_in, NT), 0.0)
        dq = jnp.where(mine, exact(dots, key_in, NN), dq)
        dk = jnp.where(mine, exact(dots, query_in, TN), dk)
        dv_ref[:, lanes] = exact(scores, grad[:, lanes], TN)
    dq = rise * dq + jnp.exp(cum) * outside
    dk = fall * dk
    dq_ref[...] = dq.astype(BF16)
    dk_ref[...] = dk
    dlog_ref[...] = query * dq - key * dk


def final_kernel(
    spot_ref,
    got_ref,
    zcols_ref,
    group_ref,
    after_ref,
    key_ref,
    value_ref,
    cum_ref,
    cols_ref,
    adj_ref,
    state_ref,
    end_ref,
    dk_in_ref,
    dv_in_ref,
    dlog_in_ref,
    dw_ref,
    dk_ref,
    dv_ref,
    dlog_ref,
):
    length, rows, _ = got_ref.shape
    keys = cum_ref.shape[1]
    half = keys // 2
    each = rows - half
    total = got_ref[0, :each, :].astype(F32)
    for k in range(1, length):
        total = total + got_ref[k, :each, :].astype(F32)
    dw_ref[...] = total
    after_z, _ = walked(
        lambda k: states_of(got_ref[k, each:, :]), jnp.exp(zcols_ref[...]), spot_ref[1], length, True
    )
    group = group_ref[...]
    tail = jnp.sum(jnp.where(iota(group.shape, 1) > spot_ref[0], group, 0.0), axis=1, keepdims=True)
    end = after_ref[...] + jnp.exp(tail) * after_z
    cols = cols_ref[...]
    middle = adj_ref[...] + jnp.exp(cols[:, 1:2]) * end
    early, late = spread_heads(middle), spread_heads(end)
    cum = cum_ref[...]
    tok = cum.shape[0]
    _, last = mids(cum)
    fade = jnp.exp(last - cum)
    key = key_ref[...].astype(F32)
    key_end = key * fade
    value = value_ref[...].astype(F32)
    dv_ref[:BLOCK, :] = (dv_in_ref[:BLOCK, :] + exact(key_end[:BLOCK], early, NN)).astype(BF16)
    dv_ref[BLOCK:, :] = (dv_in_ref[BLOCK:, :] + exact(key_end[BLOCK:], late, NN)).astype(BF16)
    more = fade * jnp.concatenate(
        [exact(value[:BLOCK], early, NT), exact(value[BLOCK:], late, NT)], axis=0
    )
    dk_ref[...] = (dk_in_ref[...] + more).astype(BF16)
    terms = dlog_in_ref[...] - key * more
    t, s = iota((tok, tok), 0), iota((tok, tok), 1)
    upper = (t <= s).astype(F32)
    end_state = jnp.exp(cols[:, 0:1] + cols[:, 1:2]) * state_ref[...] + end_ref[...]
    ones = jnp.ones((tok, VAL_DIM), F32)
    dlog_ref[...] = exact(upper, terms, NN) + exact(ones, end * end_state, NT)


def body(
    hidden_state,
    norm_gain,
    route_ids,
    route_logits,
    cotangent,
    w_gate,
    w_up,
    w_down,
    w_out,
    query_rows,
    key_rows,
    value_rows,
    log_decay,
    head_gain,
):
    tok_count, model_width = hidden_state.shape
    rank = lax.axis_index("tp")
    spot_z = lax.axis_index("sp_0")
    spot_g = lax.axis_index(GROUP)
    n_z, n_g = lax.axis_size("sp_0"), lax.axis_size(GROUP)
    experts = n_z * n_g
    part = model_width // N_TP
    keys = key_rows.shape[1]
    values = value_rows.shape[1]
    gain_row = norm_gain.reshape(1, model_width)
    head_gain_row = head_gain.reshape(1, values)
    spots = [spot_g, spot_z]

    send, place = run(
        dispatch_kernel,
        "dispatch",
        [((8 * experts, 2 * part), BF16), ((2, tok_count), jnp.int32)],
        [rank],
        hidden_state,
        gain_row,
        route_ids.T,
        route_logits,
        cotangent,
    )
    got = exchange(send.reshape(experts, 8, 2 * part), SP).reshape(8 * experts, 2 * part)
    (mine,) = run(unpack_kernel, "unpack", [((2 * experts, 2 * model_width), BF16)], [], got)

    square = ((keys, VAL_DIM), F32)
    packed, cum, cols, first, end = run(
        local_kernel,
        "local",
        [((n_g, keys + 16, VAL_DIM), BF16), ((tok_count, keys), F32), ((keys, tok_count), F32), square, square],
        [],
        key_rows,
        value_rows,
        log_decay,
    )
    got = exchange(packed, GROUP)
    packed, before_g, group_cols = run(
        group_kernel,
        "group",
        [((n_z, keys + 16, VAL_DIM), BF16), square, ((keys, n_g), F32)],
        spots,
        got,
    )
    got = exchange(packed, "sp_0")
    head_out, state_in, z_cols = run(
        forward_kernel,
        "forward",
        [((tok_count, values), F32), square, ((keys, n_z), F32)],
        spots,
        got,
        before_g,
        group_cols,
        query_rows,
        key_rows,
        value_rows,
        cum,
        cols,
        first,
    )

    left = shifted(mine, -1)
    right = shifted(mine, 1)
    far_in = shifted(left[:, :model_width], -1)
    far_grad = shifted(right[:, model_width:], 1)
    rows_in = jnp.concatenate(
        [mine[:, :model_width], right[:, :model_width], far_in, left[:, :model_width]]
    )
    rows_grad = jnp.concatenate(
        [mine[:, model_width:], right[:, model_width:], far_grad, left[:, model_width:]]
    )
    gate_w, up_w, down_w = w_gate[0], w_up[0], w_down[0]
    gate_pre = jnp.dot(rows_in, gate_w, preferred_element_type=F32)
    up_pre = jnp.dot(rows_in, up_w, preferred_element_type=F32)
    gate_sig = jax.nn.sigmoid(gate_pre)
    silu_gate = gate_pre * gate_sig
    hidden_units = (silu_gate * up_pre).astype(BF16)
    grad_hidden = jnp.einsum("rd,fd->rf", rows_grad, down_w, preferred_element_type=F32)
    grad_gate_pre = (grad_hidden * up_pre * gate_sig * (1.0 + gate_pre * (1.0 - gate_sig))).astype(BF16)
    grad_up_pre = (grad_hidden * silu_gate).astype(BF16)

    def features_of(by):
        start = ((rank + by) & 3) * part
        gate_part = lax.dynamic_slice_in_dim(gate_w, start, part, 0)
        up_part = lax.dynamic_slice_in_dim(up_w, start, part, 0)
        rows = jnp.einsum("rf,df->rd", grad_gate_pre, gate_part, preferred_element_type=F32)
        rows = rows + jnp.einsum("rf,df->rd", grad_up_pre, up_part, preferred_element_type=F32)
        return rows.astype(BF16)

    two = shifted(features_of(2), -2)
    one = shifted(features_of(1), -1)
    three = shifted(features_of(3), -3)
    own = features_of(0)
    (summed,) = run(combine_kernel, "combine", [((8 * experts, part), BF16)], [], own, one, two, three)
    returned = exchange(summed.reshape(experts, 8, part), SP).reshape(8 * experts, part)

    grad_down = jnp.einsum("rf,rd->fd", hidden_units, rows_grad, preferred_element_type=F32)
    grad_gate_w = jnp.einsum("rd,rf->df", rows_in, grad_gate_pre, preferred_element_type=F32)
    grad_up_w = jnp.einsum("rd,rf->df", rows_in, grad_up_pre, preferred_element_type=F32)

    (picked,) = run(pick_kernel, "pick", [((tok_count, part), BF16)], [], returned, place)
    half = keys // 2
    each = model_width // experts
    packed, grad_out, late_adj, _ = run(
        mixer_kernel,
        "mixer",
        [
            ((n_g, n_z * each + half, values), BF16),
            ((tok_count, values), F32),
            square,
            ((tok_count, model_width), BF16),
        ],
        [rank],
        picked,
        shifted(picked, 1),
        shifted(picked, 2),
        shifted(picked, 3),
        hidden_state,
        cotangent,
        gain_row,
        w_out,
        head_out,
        head_gain_row,
        query_rows,
        cum,
        cols,
    )

    got = exchange(packed, GROUP)
    packed, after_g = run(
        behind_kernel,
        "behind",
        [((n_z, each + half, values), BF16), square],
        spots,
        got,
        group_cols,
    )
    got = exchange(packed, "sp_0")
    grad_query, dk_part, dv_part, dlog_part = run(
        inner_kernel,
        "inner",
        [((tok_count, keys), BF16), ((tok_count, keys), F32), ((tok_count, values), F32), ((tok_count, keys), F32)],
        [],
        query_rows,
        key_rows,
        value_rows,
        cum,
        cols,
        first,
        state_in,
        grad_out,
    )
    grad_out_w, grad_key, grad_value, grad_log = run(
        final_kernel,
        "final",
        [((each, values), F32), ((tok_count, keys), BF16), ((tok_count, values), BF16), ((tok_count, keys), F32)],
        spots,
        got,
        z_cols,
        group_cols,
        after_g,
        key_rows,
        value_rows,
        cum,
        cols,
        late_adj,
        state_in,
        end,
        dk_part,
        dv_part,
        dlog_part,
    )
    return (
        grad_gate_w.astype(BF16)[None],
        grad_up_w.astype(BF16)[None],
        grad_down.astype(BF16)[None],
        grad_out_w,
        grad_query,
        grad_key,
        grad_value,
        grad_log,
    )


def solution(mesh):
    split = Mesh(mesh.devices.reshape(8, 4, 2, mesh.shape["tp"]), ("sp_0", "sp_1", "sp_2", "tp"))
    in_specs = (
        P(SP, None),
        P(),
        P(SP, None),
        P(SP, None),
        P(SP, None),
        P(SP, None, "tp"),
        P(SP, None, "tp"),
        P(SP, "tp", None),
        P(None, "tp"),
        P(SP, "tp"),
        P(SP, "tp"),
        P(SP, "tp"),
        P(SP, "tp"),
        P("tp"),
    )
    out_specs = (
        P(SP, None, "tp"),
        P(SP, None, "tp"),
        P(SP, "tp", None),
        P(SP, "tp"),
        P(SP, "tp"),
        P(SP, "tp"),
        P(SP, "tp"),
        P(SP, "tp"),
    )
    return jax.shard_map(body, mesh=split, in_specs=in_specs, out_specs=out_specs, check_vma=False)
```

```python
from typing import NamedTuple

import jax
import jax.numpy as jnp
from jax import lax
from jax.experimental import pallas as pl
from jax.experimental.pallas import tpu as pltpu
from jax.sharding import Mesh
from jax.sharding import PartitionSpec as P


KEY_DIM = 64
VAL_DIM = 128
BLOCK = 64
SP = ("sp_0", "sp_1", "sp_2")
GROUP = ("sp_1", "sp_2")
N_TP = 4
N_Z = 8
N_Y = 4
HIGH = lax.Precision.HIGHEST
EPS = 1e-06
VMEM_LIMIT = 16 * 1024 * 1024
F32 = jnp.float32
BF16 = jnp.bfloat16


def exchange(array, axis):
    return lax.all_to_all(array, axis, split_axis=0, concat_axis=0, tiled=True)


def shifted(array, by):
    return lax.ppermute(array, "tp", [((k + by) % N_TP, k) for k in range(N_TP)])


def whole():
    return pl.BlockSpec(memory_space=pltpu.VMEM)


def scalars():
    return pl.BlockSpec(memory_space=pltpu.SMEM)


class Near(NamedTuple):
    array: jax.Array


def run(kernel, outs, spots, *arrays, after=(), scratch=(), far=0):
    count = 1 + len(arrays)

    def call(*refs):
        kernel(*refs[:count], *refs[count + len(after) :])

    arrays = [
        pltpu.with_memory_space_constraint(a.array, pltpu.VMEM) if isinstance(a, Near) else a
        for a in arrays
    ]

    return pl.pallas_call(
        call,
        out_shape=tuple(
            pltpu.VMEM(shape, dtype) if rest else jax.ShapeDtypeStruct(shape, dtype)
            for shape, dtype, *rest in outs
        ),
        in_specs=[scalars()]
        + [whole()] * (len(arrays) - far)
        + [pl.BlockSpec(memory_space=pltpu.HBM)] * far
        + [pl.BlockSpec(memory_space=pltpu.HBM)] * len(after),
        out_specs=tuple(whole() for _ in outs),
        scratch_shapes=list(scratch),
        compiler_params=pltpu.CompilerParams(vmem_limit_bytes=VMEM_LIMIT),
    )(spots, *arrays, *[pltpu.with_memory_space_constraint(a, pltpu.HBM) for a in after])


def iota(shape, dim):
    return lax.broadcasted_iota(jnp.int32, shape, dim)


def exact(a, b, dims):
    return lax.dot_general(a, b, (dims, ((), ())), precision=HIGH, preferred_element_type=F32)


NN = ((1,), (0,))
NT = ((1,), (1,))
TN = ((0,), (0,))


def paired(a, b, dims):
    return lax.dot_general(a, b, (dims, ((), ())), preferred_element_type=F32)


def slot_rows(rank, ids, experts, tok):
    eye = iota((experts, tok), 0)
    hot = [(eye == ids[r : r + 1, :]).astype(F32) for r in range(2)]
    earlier = (iota((tok, tok), 0) < iota((tok, tok), 1)).astype(F32)
    before = paired(hot[0] + hot[1], earlier, NN)
    kept, places = [], []
    for r in range(2):
        slot = jnp.sum(before * hot[r], axis=0, keepdims=True).astype(jnp.int32)
        block = slot >> 1
        first = 8 * ids[r : r + 1, :] + (slot & 1)
        kept.append(jnp.where(block == rank, first, -8))
        places.append(first + 2 * ((block - rank) & 3))
    return kept, places


def inputs_kernel(
    rank_ref, hidden_hbm, gain_hbm, ids_hbm, send_ref, place_ref, kept_ref, hidden_ref, gain_ref, ids_ref, sems
):
    copies = [
        pltpu.make_async_copy(source, target, sems.at[k])
        for k, (source, target) in enumerate(
            ((hidden_hbm, hidden_ref), (gain_hbm, gain_ref), (ids_hbm, ids_ref))
        )
    ]
    for copy in copies:
        copy.start()
    for copy in copies:
        copy.wait()
    tok, width = hidden_ref.shape
    quarter = width // 4
    state = hidden_ref[...].astype(F32)
    scale = lax.rsqrt(jnp.mean(state * state, axis=-1, keepdims=True) + EPS)
    normed = ((state * scale) * gain_ref[...]).astype(BF16)
    rows_all = send_ref.shape[0]
    kept, places = slot_rows(rank_ref[4], ids_ref[...], rows_all // 8, tok)
    place_ref[...] = jnp.concatenate(places, axis=0)
    kept_ref[...] = jnp.concatenate(kept, axis=0)
    rows = iota((rows_all, 4 * tok), 0)
    kept = [jnp.concatenate([k + 2 * h for h in range(4)], axis=1) for k in kept]
    pick = ((rows == kept[0]) | (rows == kept[1])).astype(F32).astype(BF16)
    quarters = [normed[:, h * quarter : (h + 1) * quarter] for h in range(4)]
    send_ref[...] = paired(pick, jnp.concatenate(quarters, axis=0), NN).astype(BF16)


def grads_kernel(_, logits_ref, cot_ref, kept_ref, send_ref):
    tok, width = cot_ref.shape
    quarter = width // 4
    logits = jnp.transpose(jnp.concatenate([logits_ref[...]] * 4, axis=0))
    l0, l1 = logits[:, 0:1], logits[:, 1:2]
    top = jnp.maximum(l0, l1)
    e0, e1 = jnp.exp(l0 - top), jnp.exp(l1 - top)
    norm = e0 + e1
    cot = cot_ref[...].astype(F32)
    grads = [((e / norm) * cot).astype(BF16) for e in (e0, e1)]
    quarters = [g[:, h * quarter : (h + 1) * quarter] for h in range(4) for g in grads]
    kept = [kept_ref[r : r + 1, :] + 2 * h for h in range(4) for r in range(2)]
    pick = iota((send_ref.shape[0], 8 * tok), 0) == jnp.concatenate(kept, axis=1)
    pick = pick.astype(F32).astype(BF16)
    send_ref[...] = paired(pick, jnp.concatenate(quarters, axis=0), NN).astype(BF16)


def unpack_kernel(_, got_ref, *out_refs):
    got = got_ref[...]
    rows = got.shape[0] // 4
    quarter = got.shape[1]
    each = rows // len(out_refs)
    line = iota((rows, got.shape[0]), 0)
    col = iota((rows, got.shape[0]), 1)
    base = col - 8 * (line >> 1) - (line & 1)
    for h in range(4):
        pick = (base == 2 * h).astype(F32).astype(BF16)
        block = paired(pick, got, NN).astype(BF16)
        for k, ref in enumerate(out_refs):
            ref[:, h * quarter : (h + 1) * quarter] = block[k * each : (k + 1) * each]


def assembled(pieces, first=0, into=None, rows=0):
    each, width = pieces[0].shape
    rows = into.shape[0] if into is not None else rows

    def kernel(*refs):
        out_ref, sems = refs[-2], refs[-1]
        copies = [
            pltpu.make_async_copy(refs[k], out_ref.at[pl.ds(first + k * each, each), :], sems.at[k])
            for k in range(len(pieces))
        ]
        for copy in copies:
            copy.start()
        for copy in copies:
            copy.wait()

    inputs = list(pieces) + ([] if into is None else [into])
    return pl.pallas_call(
        kernel,
        out_shape=jax.ShapeDtypeStruct((rows, width), BF16),
        in_specs=[pl.BlockSpec(memory_space=pl.ANY)] * len(inputs),
        out_specs=pl.BlockSpec(memory_space=pl.ANY),
        scratch_shapes=[pltpu.SemaphoreType.DMA((len(pieces),))],
        input_output_aliases={} if into is None else {len(pieces): 0},
        compiler_params=pltpu.CompilerParams(vmem_limit_bytes=VMEM_LIMIT),
    )(*inputs)


def combine_kernel(_, *refs):
    arrays, out_ref = refs[:-1], refs[-1]
    rows = arrays[0].shape[0] // 4
    line = iota((4 * rows, 4 * rows), 0)
    col = iota((4 * rows, 4 * rows), 1)
    within = col & (rows - 1)
    spread = line == 8 * (within >> 1) + (within & 1) + 2 * (col // rows)
    place = (0, 1, 3, 2)
    blocks = []
    for k in range(4):
        acc = None
        for by in range(4):
            at = place[(k + by) % 4] * rows
            block = arrays[by][at : at + rows].astype(F32)
            acc = block if acc is None else acc + block
        blocks.append(acc.astype(BF16))
    spread = spread.astype(F32).astype(BF16)
    out_ref[...] = paired(spread, jnp.concatenate(blocks, axis=0), NN).astype(BF16)


def weights_kernel(
    _, in_ref, grad_ref, units_ref, gate_pre_ref, up_pre_ref, gate_ref, up_ref, down_ref
):
    width = gate_ref.shape[1]
    both = jnp.concatenate([gate_pre_ref[...], up_pre_ref[...]], axis=1)
    units = units_ref[...]
    block = 512

    def step(k, carry):
        at = pl.ds(pl.multiple_of(k * block, block), block)
        out = paired(in_ref[:, at], both, TN).astype(BF16)
        gate_ref[at, :] = out[:, :width]
        up_ref[at, :] = out[:, width:]
        down_ref[:, at] = paired(units, grad_ref[:, at], TN).astype(BF16)
        return carry

    lax.fori_loop(0, in_ref.shape[1] // block, step, 0)


def pick_kernel(_, returned_ref, place_ref, out_ref):
    tok = out_ref.shape[0]
    slots = iota((returned_ref.shape[0], tok), 0)
    here = ((slots == place_ref[0:1, :]) | (slots == place_ref[1:2, :])).astype(F32).astype(BF16)
    out_ref[...] = paired(here, returned_ref[...], TN).astype(BF16)


def by_head(x):
    half = x.shape[0] // 2
    return jnp.concatenate([x[:half, :VAL_DIM], x[half:, VAL_DIM:]], axis=0)


def spread_heads(x):
    half = x.shape[0] // 2
    zero = jnp.zeros((half, VAL_DIM), F32)
    return jnp.concatenate(
        [jnp.concatenate([x[:half], zero], axis=1), jnp.concatenate([zero, x[half:]], axis=1)], axis=0
    )


def same_block(t, s):
    return (t // BLOCK) == (s // BLOCK)


def mids(cum):
    tok, keys = cum.shape
    row = iota((tok, keys), 0)
    mid = jnp.where(row < BLOCK, cum[BLOCK // 2 : BLOCK // 2 + 1], cum[BLOCK + BLOCK // 2 : BLOCK + BLOCK // 2 + 1])
    last = jnp.where(row < BLOCK, cum[BLOCK - 1 : BLOCK], cum[2 * BLOCK - 1 : 2 * BLOCK])
    return mid, last


def pack_state(out_ref, state, log_row):
    keys = state.shape[0]
    high = log_row.astype(BF16).astype(F32)
    rest = log_row - high
    middle = rest.astype(BF16).astype(F32)
    low = rest - middle
    line = iota((16, state.shape[1]), 0)
    extra = jnp.where(line == 0, high, jnp.where(line == 1, middle, jnp.where(line == 2, low, 0.0)))
    block = state.astype(BF16)
    extra = extra.astype(BF16)
    for k in range(out_ref.shape[0]):
        out_ref[k, :keys, :] = block
        out_ref[k, keys:, :] = extra


def local_kernel(_, key_ref, value_ref, log_ref, pack_ref, cum_ref, cols_ref, first_ref, end_ref):
    tok, _ = key_ref.shape
    logs = log_ref[...]
    t, s = iota((tok, tok), 0), iota((tok, tok), 1)
    lower = ((t >= s) & same_block(t, s)).astype(F32)
    cum = exact(lower, logs, NN)
    cum_ref[...] = cum
    _, last = mids(cum)
    chosen = ((t // BLOCK) == s).astype(F32)
    cols = exact(logs, chosen, TN)
    cols_ref[...] = cols
    key_end = key_ref[...].astype(F32) * jnp.exp(last - cum)
    value = value_ref[...].astype(F32)
    first = by_head(exact(key_end[:BLOCK], value[:BLOCK], TN))
    second = by_head(exact(key_end[BLOCK:], value[BLOCK:], TN))
    end = jnp.exp(cols[:, 1:2]) * first + second
    first_ref[...] = first
    end_ref[...] = end
    pack_state(pack_ref, end, cum[BLOCK - 1 : BLOCK] + cum[2 * BLOCK - 1 : 2 * BLOCK])


def log_rows(got_ref, keys):
    return jnp.concatenate(
        [
            jnp.sum(got_ref[k, keys:, :].astype(F32), axis=0, keepdims=True)
            for k in range(got_ref.shape[0])
        ],
        axis=0,
    )


def walked(term_of, decays, position, length, reverse):
    carried = jnp.zeros((decays.shape[0], VAL_DIM), F32)
    here = carried
    for k in reversed(range(length)) if reverse else range(length):
        here = jnp.where(position == k, carried, here)
        carried = decays[:, k : k + 1] * carried + term_of(k)
    return here, carried


def group_kernel(spot_ref, got_ref, pack_ref, before_ref, cols_ref):
    length, _, keys = got_ref.shape
    rows = log_rows(got_ref, keys)
    cols = jnp.transpose(rows)
    cols_ref[...] = cols
    here, carried = walked(
        lambda k: got_ref[k, :keys, :].astype(F32), jnp.exp(cols), spot_ref[0], length, False
    )
    before_ref[...] = here
    pack_state(pack_ref, carried, jnp.sum(rows, axis=0, keepdims=True))


def forward_kernel(
    spot_ref,
    got_ref,
    before_ref,
    group_ref,
    query_ref,
    key_ref,
    value_ref,
    cum_ref,
    cols_ref,
    first_ref,
    out_ref,
    state_ref,
    zcols_ref,
):
    length, _, keys = got_ref.shape
    cols = jnp.transpose(log_rows(got_ref, keys))
    zcols_ref[...] = cols
    before_z, _ = walked(
        lambda k: got_ref[k, :keys, :].astype(F32), jnp.exp(cols), spot_ref[1], length, False
    )
    group = group_ref[...]
    lead = jnp.sum(jnp.where(iota(group.shape, 1) < spot_ref[0], group, 0.0), axis=1, keepdims=True)
    state = before_ref[...] + jnp.exp(lead) * before_z
    state_ref[...] = state
    cum = cum_ref[...]
    tok = cum.shape[0]
    mid, _ = mids(cum)
    query = query_ref[...].astype(F32)
    query_in = query * jnp.exp(cum - mid)
    key_in = key_ref[...].astype(F32) * jnp.exp(mid - cum)
    start = query * jnp.exp(cum)
    t, s = iota((tok, tok), 0), iota((tok, tok), 1)
    causal = (t >= s) & same_block(t, s)
    lane = iota((tok, keys), 1) // KEY_DIM
    later = first_ref[...] + jnp.exp(cols_ref[:, 0:1]) * state
    outside = jnp.concatenate(
        [exact(start[:BLOCK], spread_heads(state), NN), exact(start[BLOCK:], spread_heads(later), NN)],
        axis=0,
    )
    out_ref[...] = outside

    def step(h, carry):
        lanes = pl.ds(pl.multiple_of(h * VAL_DIM, VAL_DIM), VAL_DIM)
        scores = exact(jnp.where(lane == h, query_in, 0.0), key_in, NT)
        scores = jnp.where(causal, scores, 0.0)
        value = value_ref[:, lanes].astype(F32)
        out_ref[:, lanes] = exact(scores, value, NN) + out_ref[:, lanes]
        return carry

    lax.fori_loop(0, 2, step, 0)


def head_norm(head_out):
    normed, scale = [], []
    for h in range(2):
        x = head_out[:, h * VAL_DIM : (h + 1) * VAL_DIM]
        r = lax.rsqrt(jnp.mean(x * x, axis=-1, keepdims=True) + EPS)
        scale.append(r)
        normed.append(x * r)
    return normed, scale


def mixer_kernel(
    rank_ref,
    own_ref,
    one_ref,
    two_ref,
    three_ref,
    hidden_ref,
    cot_ref,
    gain_ref,
    w_out_ref,
    head_ref,
    head_gain_ref,
    query_ref,
    cum_ref,
    cols_ref,
    give_ref,
    keep_ref,
    grad_ref,
    adj_ref,
    local_ref,
    mixed_ref,
    out_scr,
):
    rank = rank_ref[4]
    tok, width = hidden_ref.shape
    part = width // 4
    state = hidden_ref[...].astype(F32)
    scale = lax.rsqrt(jnp.mean(state * state, axis=-1, keepdims=True) + EPS)
    parts = (own_ref, one_ref, two_ref, three_ref)
    inner = jnp.zeros((tok, 1), F32)
    for k in range(4):
        at = pl.multiple_of(((rank + k) & 3) * part, part)
        unit = hidden_ref[:, pl.ds(at, part)].astype(F32) * scale
        u = parts[k][...].astype(F32) * gain_ref[:, pl.ds(at, part)]
        inner = inner + jnp.sum(u * unit, axis=-1, keepdims=True)
    inner = inner / width
    grad_mix = None
    for k in range(4):
        at = pl.multiple_of(((rank + k) & 3) * part, part)
        unit = hidden_ref[:, pl.ds(at, part)].astype(F32) * scale
        u = parts[k][...].astype(F32) * gain_ref[:, pl.ds(at, part)]
        mixed = (cot_ref[:, pl.ds(at, part)].astype(F32) + scale * (u - unit * inner)).astype(BF16)
        mixed_ref[:, pl.ds(at, part)] = mixed
        term = paired(mixed, w_out_ref[pl.ds(at, part), :], NN)
        grad_mix = term if grad_mix is None else grad_mix + term
    grad_mix = grad_mix.astype(BF16).astype(F32)
    head_gain = head_gain_ref[...]
    normed, head_scale = head_norm(head_ref[...])
    out = []
    for h in range(2):
        lanes = slice(h * VAL_DIM, (h + 1) * VAL_DIM)
        u = grad_mix[:, lanes] * head_gain[:, lanes]
        n = normed[h]
        out.append(head_scale[h] * (u - n * jnp.mean(u * n, axis=-1, keepdims=True)))
    grad = jnp.concatenate(out, axis=1)
    grad_ref[...] = grad
    start = query_ref[...].astype(F32) * jnp.exp(cum_ref[...])
    early = by_head(exact(start[:BLOCK], grad[:BLOCK], TN))
    late = by_head(exact(start[BLOCK:], grad[BLOCK:], TN))
    adj_ref[...] = late
    local = jnp.exp(cols_ref[:, 0:1]) * late + early
    local_ref[...] = local
    local = local.astype(BF16)
    half = local.shape[0] // 2
    mixed_out = jnp.concatenate(
        [normed[h] * head_gain[:, h * VAL_DIM : (h + 1) * VAL_DIM] for h in range(2)], axis=1
    ).astype(BF16)

    def step(k, carry):
        at = pl.ds(pl.multiple_of(k * part, part), part)
        out_scr[at, :] = paired(mixed_ref[:, at], mixed_out, TN).astype(BF16)
        return carry

    lax.fori_loop(0, 4, step, 0)
    core = rank_ref[2]
    rows = keep_ref.shape[0]
    each = rows // (N_Y * N_Z)

    def deal(z, carry):
        for y in range(N_Y):
            base = (z * N_Y + y) * 2
            at = pl.ds(pl.multiple_of((y * N_Z + z) * each, each), each)
            mine = pl.multiple_of((base + core) * each, each)
            other = pl.multiple_of((base + 1 - core) * each, each)
            keep_ref[at, :] = out_scr[pl.ds(mine, each), :]
            give_ref[at, :] = out_scr[pl.ds(other, each), :]
        return carry

    lax.fori_loop(0, N_Z, deal, 0)
    give_ref[rows:, :] = jnp.concatenate([local[:half], local[half:]], axis=1)


def states_of(rows):
    return jnp.concatenate([rows[:, :VAL_DIM], rows[:, VAL_DIM:]], axis=0).astype(F32)


def pair_kernel(spot_ref, keep_ref, got_ref, local_ref, cols_ref, *out_refs):
    own_ref, parts, (near_ref, pair_ref) = out_refs[0], out_refs[1:4], out_refs[4:]
    core, y = spot_ref[2], spot_ref[3]
    rows = keep_ref.shape[0]
    per = rows // N_Y
    half = local_ref.shape[0] // 2
    other = states_of(got_ref[rows:, :])
    local = local_ref[...]
    last = core == 1
    first_term = jnp.where(last, other, local)
    second_term = jnp.where(last, local, other)
    near_ref[...] = jnp.where(last, 0.0, other)
    lane = iota(cols_ref.shape, 1)
    logs = jnp.sum(jnp.where(lane == 2 * y, cols_ref[...], 0.0), axis=1, keepdims=True)
    pair = first_term + jnp.exp(logs) * second_term
    pair_ref[...] = pair
    pair = pair.astype(BF16)
    state_rows = jnp.concatenate([pair[:half], pair[half:]], axis=1)
    for by in range(N_Y):
        at = pl.multiple_of(((y + by) & 3) * per, per)
        total = keep_ref[pl.ds(at, per), :].astype(F32) + got_ref[pl.ds(at, per), :].astype(F32)
        if by == 0:
            own_ref[...] = total
        else:
            parts[by - 1][:per, :] = total.astype(BF16)
            parts[by - 1][per:, :] = state_rows


def behind_kernel(spot_ref, own_ref, one_ref, two_ref, three_ref, near_ref, pair_ref, cols_ref, pack_ref, after_ref):
    core, y = spot_ref[2], spot_ref[3]
    per = own_ref.shape[0]
    half = near_ref.shape[0] // 2
    each = per // N_Z
    total = own_ref[...]
    pairs = [pair_ref[...]]
    for ref in (one_ref, two_ref, three_ref):
        total = total + ref[:per, :].astype(F32)
        pairs.append(states_of(ref[per:, :]))
    total = total.astype(BF16)
    decays = jnp.exp(cols_ref[...])
    carried = jnp.zeros(near_ref.shape, F32)
    here = carried
    for k in reversed(range(N_Y)):
        here = jnp.where(y == k, carried, here)
        term = pairs[0]
        for by in range(1, N_Y):
            term = jnp.where(((y - by) & 3) == k, pairs[by], term)
        carried = (decays[:, 2 * k : 2 * k + 1] * decays[:, 2 * k + 1 : 2 * k + 2]) * carried + term
    lane = iota(cols_ref.shape, 1)
    logs = jnp.sum(jnp.where(lane == 2 * y + 1, cols_ref[...], 0.0), axis=1, keepdims=True)
    after_ref[...] = near_ref[...] + jnp.where(core == 1, 1.0, jnp.exp(logs)) * here
    carried = carried.astype(BF16)
    state_rows = jnp.concatenate([carried[:half], carried[half:]], axis=1)
    for z in range(N_Z):
        pack_ref[z, :each, :] = total[z * each : (z + 1) * each]
        pack_ref[z, each:, :] = state_rows


def inner_kernel(
    _,
    query_ref,
    key_ref,
    value_ref,
    cum_ref,
    cols_ref,
    first_ref,
    state_ref,
    grad_ref,
    dq_ref,
    dk_ref,
    dv_ref,
    dlog_ref,
):
    cum = cum_ref[...]
    tok, keys = cum.shape
    mid, _ = mids(cum)
    query, key = query_ref[...].astype(F32), key_ref[...].astype(F32)
    rise, fall = jnp.exp(cum - mid), jnp.exp(mid - cum)
    query_in, key_in = query * rise, key * fall
    grad = grad_ref[...]
    t, s = iota((tok, tok), 0), iota((tok, tok), 1)
    causal = (t >= s) & same_block(t, s)
    lane = iota((tok, keys), 1) // KEY_DIM
    state = state_ref[...]
    later = first_ref[...] + jnp.exp(cols_ref[:, 0:1]) * state
    outside = jnp.concatenate(
        [exact(grad[:BLOCK], spread_heads(state), NT), exact(grad[BLOCK:], spread_heads(later), NT)],
        axis=0,
    )
    zero = jnp.zeros((tok, keys), F32)

    def step(h, carry):
        dq, dk = carry
        lanes = pl.ds(pl.multiple_of(h * VAL_DIM, VAL_DIM), VAL_DIM)
        mine = lane == h
        grad_h = grad_ref[:, lanes]
        dots = jnp.where(causal, exact(grad_h, value_ref[:, lanes].astype(F32), NT), 0.0)
        scores = jnp.where(causal, exact(jnp.where(mine, query_in, 0.0), key_in, NT), 0.0)
        dv_ref[:, lanes] = exact(scores, grad_h, TN)
        return (
            jnp.where(mine, exact(dots, key_in, NN), dq),
            jnp.where(mine, exact(dots, query_in, TN), dk),
        )

    dq, dk = lax.fori_loop(0, 2, step, (zero, zero))
    dq = rise * dq + jnp.exp(cum) * outside
    dk = fall * dk
    dq_ref[...] = dq.astype(BF16)
    dk_ref[...] = dk
    dlog_ref[...] = query * dq - key * dk


def final_kernel(
    spot_ref,
    got_ref,
    zcols_ref,
    group_ref,
    after_ref,
    key_ref,
    value_ref,
    cum_ref,
    cols_ref,
    adj_ref,
    state_ref,
    end_ref,
    dk_in_ref,
    dv_in_ref,
    dlog_in_ref,
    dw_ref,
    dk_ref,
    dv_ref,
    dlog_ref,
):
    length, rows, _ = got_ref.shape
    keys = cum_ref.shape[1]
    half = keys // 2
    each = rows - half
    total = got_ref[0, :each, :].astype(F32)
    for k in range(1, length):
        total = total + got_ref[k, :each, :].astype(F32)
    dw_ref[...] = total
    after_z, _ = walked(
        lambda k: states_of(got_ref[k, each:, :]), jnp.exp(zcols_ref[...]), spot_ref[1], length, True
    )
    group = group_ref[...]
    tail = jnp.sum(jnp.where(iota(group.shape, 1) > spot_ref[0], group, 0.0), axis=1, keepdims=True)
    end = after_ref[...] + jnp.exp(tail) * after_z
    cols = cols_ref[...]
    middle = adj_ref[...] + jnp.exp(cols[:, 1:2]) * end
    early, late = spread_heads(middle), spread_heads(end)
    cum = cum_ref[...]
    tok = cum.shape[0]
    _, last = mids(cum)
    fade = jnp.exp(last - cum)
    key = key_ref[...].astype(F32)
    key_end = key * fade
    value = value_ref[...].astype(F32)
    dv_ref[:BLOCK, :] = (dv_in_ref[:BLOCK, :] + exact(key_end[:BLOCK], early, NN)).astype(BF16)
    dv_ref[BLOCK:, :] = (dv_in_ref[BLOCK:, :] + exact(key_end[BLOCK:], late, NN)).astype(BF16)
    more = fade * jnp.concatenate(
        [exact(value[:BLOCK], early, NT), exact(value[BLOCK:], late, NT)], axis=0
    )
    dk_ref[...] = (dk_in_ref[...] + more).astype(BF16)
    terms = dlog_in_ref[...] - key * more
    t, s = iota((tok, tok), 0), iota((tok, tok), 1)
    upper = (t <= s).astype(F32)
    end_state = jnp.exp(cols[:, 0:1] + cols[:, 1:2]) * state_ref[...] + end_ref[...]
    ones = jnp.ones((tok, VAL_DIM), F32)
    dlog_ref[...] = exact(upper, terms, NN) + exact(ones, end * end_state, NT)


def layer(
    hidden_state,
    norm_gain,
    route_ids,
    route_logits,
    cotangent,
    w_gate,
    w_up,
    w_down,
    w_out,
    query_rows,
    key_rows,
    value_rows,
    log_decay,
    head_gain,
):
    tok_count, model_width = hidden_state.shape
    rank = lax.axis_index("tp")
    spot_z = lax.axis_index("sp_0")
    spot_g = lax.axis_index(GROUP)
    n_z, n_g = lax.axis_size("sp_0"), lax.axis_size(GROUP)
    experts = n_z * n_g
    part = model_width // N_TP
    keys = key_rows.shape[1]
    values = value_rows.shape[1]
    gain_row = norm_gain.reshape(1, model_width)
    head_gain_row = head_gain.reshape(1, values)
    spot_c, spot_y = lax.axis_index("sp_2"), lax.axis_index("sp_1")
    spots = jnp.stack([spot_g, spot_z, spot_c, spot_y, rank])

    send_in, place, kept = run(
        inputs_kernel,
        [((8 * experts, part), BF16), ((2, tok_count), jnp.int32, 1), ((2, tok_count), jnp.int32, 1)],
        spots,
        *[
            pltpu.with_memory_space_constraint(a, pltpu.HBM)
            for a in (hidden_state, gain_row, route_ids.T)
        ],
        scratch=[
            pltpu.VMEM((tok_count, model_width), BF16),
            pltpu.VMEM((1, model_width), F32),
            pltpu.VMEM((2, tok_count), jnp.int32),
            pltpu.SemaphoreType.DMA((3,)),
        ],
        far=3,
    )
    got_in = exchange(send_in.reshape(experts, 8, part), SP).reshape(8 * experts, part)
    (send_grad,) = run(
        grads_kernel, [((8 * experts, part), BF16)], spots, route_logits.T, Near(cotangent), Near(kept)
    )
    square = ((keys, VAL_DIM), F32, 1)
    packed, cum, cols, first, end = run(
        local_kernel,
        [
            ((n_g, keys + 16, VAL_DIM), BF16),
            ((tok_count, keys), F32, 1),
            ((keys, tok_count), F32, 1),
            square,
            square,
        ],
        spots,
        key_rows,
        value_rows,
        log_decay,
    )
    got_grad = exchange(send_grad.reshape(experts, 8, part), SP).reshape(8 * experts, part)

    def ring(got):
        upper, lower = run(unpack_kernel, [((experts, model_width), BF16, 1)] * 2, spots, Near(got))
        left_upper, right_lower = shifted(upper, -1), shifted(lower, 1)
        left_lower, right_upper = shifted(lower, -1), shifted(upper, 1)
        far = (shifted(left_upper, -1), shifted(right_lower, 1))
        return (upper, lower, right_upper, right_lower, left_upper, left_lower), far

    near_in, far_in = ring(got_in)
    near, far = ring(got_grad)
    got_group = exchange(packed, GROUP)

    gate_w, up_w, down_w = w_gate[0], w_up[0], w_down[0]
    hidden = gate_w.shape[1]
    rows_all = 8 * experts
    rows_in = assembled(near_in + far_in, rows=rows_all)
    gate_pre = jnp.dot(rows_in, gate_w, preferred_element_type=F32)
    up_pre = jnp.dot(rows_in, up_w, preferred_element_type=F32)
    gate_sig = jax.nn.sigmoid(gate_pre)
    silu_gate = gate_pre * gate_sig
    hidden_units = (silu_gate * up_pre).astype(BF16)
    rows_grad = assembled(near, rows=rows_all)
    rows_grad = assembled(far, first=6 * experts, into=rows_grad)
    grad_hidden = jnp.einsum("rd,fd->rf", rows_grad, down_w, preferred_element_type=F32)
    grad_gate_pre = (grad_hidden * up_pre * gate_sig * (1.0 + gate_pre * (1.0 - gate_sig))).astype(BF16)
    grad_up_pre = (grad_hidden * silu_gate).astype(BF16)

    def features_of(by):
        start = ((rank + by) & 3) * part
        gate_part = lax.dynamic_slice_in_dim(gate_w, start, part, 0)
        up_part = lax.dynamic_slice_in_dim(up_w, start, part, 0)
        rows = jnp.einsum("rf,df->rd", grad_gate_pre, gate_part, preferred_element_type=F32)
        rows = rows + jnp.einsum("rf,df->rd", grad_up_pre, up_part, preferred_element_type=F32)
        return rows.astype(BF16)

    two = shifted(features_of(2), -2)
    one = shifted(features_of(1), -1)
    three = shifted(features_of(3), -3)
    own = features_of(0)
    packed, before_g, group_cols = run(
        group_kernel,
        [((n_z, keys + 16, VAL_DIM), BF16), square, ((keys, n_g), F32, 1)],
        spots,
        Near(got_group),
    )
    got = exchange(packed, "sp_0")
    head_out, state_in, z_cols = run(
        forward_kernel,
        [((tok_count, values), F32, 1), square, ((keys, n_z), F32, 1)],
        spots,
        Near(got),
        Near(before_g),
        Near(group_cols),
        query_rows,
        key_rows,
        value_rows,
        Near(cum),
        Near(cols),
        Near(first),
    )
    (summed,) = run(
        combine_kernel,
        [((rows_all, part), BF16)],
        spots,
        Near(own),
        Near(one),
        Near(two),
        Near(three),
    )
    returned = exchange(summed.reshape(experts, 8, part), SP).reshape(8 * experts, part)

    rows_in, rows_grad, hidden_units, grad_gate_pre, grad_up_pre, _ = lax.optimization_barrier(
        (rows_in, rows_grad, hidden_units, grad_gate_pre, grad_up_pre, summed)
    )
    grad_gate_w, grad_up_w, grad_down = run(
        weights_kernel,
        [((model_width, hidden), BF16)] * 2 + [((hidden, model_width), BF16)],
        spots,
        rows_in,
        rows_grad,
        hidden_units,
        grad_gate_pre,
        grad_up_pre,
    )

    (picked,) = run(
        pick_kernel,
        [((tok_count, part), BF16, 1)],
        spots,
        Near(returned),
        Near(place),
        after=(grad_down, grad_gate_w, grad_up_w),
    )
    half = keys // 2
    each = model_width // experts
    rows_y = model_width // 2
    per = rows_y // N_Y
    give, keep, grad_out, late_adj, local_adj, _ = run(
        mixer_kernel,
        [
            ((rows_y + half, values), BF16, 1),
            ((rows_y, values), BF16, 1),
            ((tok_count, values), F32, 1),
            square,
            square,
            ((tok_count, model_width), BF16, 1),
        ],
        spots,
        Near(picked),
        Near(shifted(picked, 1)),
        Near(shifted(picked, 2)),
        Near(shifted(picked, 3)),
        Near(hidden_state),
        Near(cotangent),
        gain_row,
        Near(w_out),
        Near(head_out),
        head_gain_row,
        query_rows,
        Near(cum),
        Near(cols),
        scratch=[pltpu.VMEM((model_width, values), BF16)],
    )

    got = lax.ppermute(give, "sp_2", [(0, 1), (1, 0)])
    own, one, two, three, near, pair = run(
        pair_kernel,
        [((per, values), F32, 1)] + [((per + half, values), BF16, 1)] * 3 + [square] * 2,
        spots,
        Near(keep),
        Near(got),
        Near(local_adj),
        Near(group_cols),
    )
    one, two, three = (
        lax.ppermute(x, "sp_1", [(k, (k + by) % N_Y) for k in range(N_Y)])
        for by, x in ((1, one), (2, two), (3, three))
    )
    packed, after_g = run(
        behind_kernel,
        [((n_z, each + half, values), BF16), square],
        spots,
        Near(own),
        Near(one),
        Near(two),
        Near(three),
        Near(near),
        Near(pair),
        Near(group_cols),
    )
    got = exchange(packed, "sp_0")
    grad_query, dk_part, dv_part, dlog_part = run(
        inner_kernel,
        [
            ((tok_count, keys), BF16),
            ((tok_count, keys), F32, 1),
            ((tok_count, values), F32, 1),
            ((tok_count, keys), F32, 1),
        ],
        spots,
        query_rows,
        key_rows,
        value_rows,
        Near(cum),
        Near(cols),
        Near(first),
        Near(state_in),
        Near(grad_out),
    )
    grad_out_w, grad_key, grad_value, grad_log = run(
        final_kernel,
        [((each, values), F32), ((tok_count, keys), BF16), ((tok_count, values), BF16), ((tok_count, keys), F32)],
        spots,
        Near(got),
        Near(z_cols),
        Near(group_cols),
        Near(after_g),
        Near(key_rows),
        Near(value_rows),
        Near(cum),
        Near(cols),
        Near(late_adj),
        Near(state_in),
        Near(end),
        Near(dk_part),
        Near(dv_part),
        Near(dlog_part),
    )
    return (
        grad_gate_w[None],
        grad_up_w[None],
        grad_down[None],
        grad_out_w,
        grad_query,
        grad_key,
        grad_value,
        grad_log,
    )


def solution(mesh):
    split = Mesh(mesh.devices.reshape(8, 4, 2, mesh.shape["tp"]), ("sp_0", "sp_1", "sp_2", "tp"))
    in_specs = (
        P(SP, None),
        P(),
        P(SP, None),
        P(SP, None),
        P(SP, None),
        P(SP, None, "tp"),
        P(SP, None, "tp"),
        P(SP, "tp", None),
        P(None, "tp"),
        P(SP, "tp"),
        P(SP, "tp"),
        P(SP, "tp"),
        P(SP, "tp"),
        P("tp"),
    )
    out_specs = (
        P(SP, None, "tp"),
        P(SP, None, "tp"),
        P(SP, "tp", None),
        P(SP, "tp"),
        P(SP, "tp"),
        P(SP, "tp"),
        P(SP, "tp"),
        P(SP, "tp"),
    )
    return jax.shard_map(layer, mesh=split, in_specs=in_specs, out_specs=out_specs, check_vma=False)
```
